32 devices in a mesh: ep: 8 (over z, x), tp: 4 (over y, core).
Axes of the slice: x: 2, y: 2, z: 4, core: 2. Of those that a mesh axis runs over, the one named last changes fastest.
Arguments:
- filter_value: bfloat16 [8192, 1024], P(('ep', 'tp')), may hold values from -6 to 6
- filter_gate: bfloat16 [8192, 1024], P(('ep', 'tp')), may hold values from -9 to 9
- filter_taps: float32 [31, 1024], replicated, may hold values from -1 to 1
- filter_bias: float32 [1024], replicated, may hold values from -3 to 3
- norm_gain: float32 [1024], replicated, may hold values from 0.1 to 1.9
- norm_shift: float32 [1024], replicated, may hold values from -3 to 3
- out_weight: bfloat16 [1024, 2048], replicated, may hold values from -0.1875 to 0.1875
- out_bias: float32 [2048], replicated, may hold values from -3 to 3
- expert_input: bfloat16 [2048, 2048], P('ep'), may hold values from -6 to 6
- expert_gain: float32 [2048], replicated, may hold values from 0.1 to 1.9
- route_experts: int32 [2048, 2], P('ep'), may hold values from 0 to 7, all different within a row; in each aligned block of 256 rows (0 to 255, 256 to 511, ...) at most 128 rows name the same one
- route_weights: float32 [2048, 2], P('ep'), may hold values from 0.2 to 1
- gate_weights: bfloat16 [8, 2048, 2048], P('ep', None, 'tp'), may hold values from -0.375 to 0.375
- up_weights: bfloat16 [8, 2048, 2048], P('ep', None, 'tp'), may hold values from -0.375 to 0.375
- down_weights: bfloat16 [8, 2048, 2048], P('ep', 'tp'), may hold values from -0.0234375 to 0.0234375
Outputs:
- mixer_out: bfloat16 [8192, 2048], P(('ep', 'tp'))
- expert_out: bfloat16 [2048, 2048], P('ep', 'tp')
The draws below stay inside these ranges and needn't reach their ends.
Inputs may be any that keep to these rules, and one draw needn't show every extreme that they name: `route_experts`: each row names 2 different experts. Within the rows of one index of ep (aligned blocks of 256 rows) no expert is named by more than 128 rows, a bound that some block reaches.
All inputs are finite; a program needn't handle non-finite values.
Results may differ from the reference program's by a relative error of at most 0.012.
Values may be sent and summed in bfloat16 or wider, within the bound.
No kernel may reach another device: no remote copies, remote signals or barrier semaphores. Data moves between devices by JAX's collectives and lax.ppermute only.
A program may use at most 128 MiB of HBM per device.

```python
import math
import jax
import jax.numpy as jnp
import numpy as np
from jax import lax

D = 2048
CHANNELS = 1024
TAPS = 31
HIDDEN_SIZE = 2048
TOPK = 2
ROUTE_DEV = 256
EXPERTS = 8
CAPACITY = 128
MIX_TOKENS = 8192
ROUTE_TOKENS = 2048
N_EP = 8
N_TP = 4


def level_of(rng, shape, split, low, top_value):
    def one(axis_at, parts):
        draws = jax.random.uniform(jax.random.fold_in(jax.random.fold_in(rng, 6), axis_at), (parts,), jnp.float32, low / len(split), top_value / len(split))
        return jnp.repeat(jnp.exp(draws), shape[axis_at] // parts).reshape((-1,) + (1,) * (len(shape) - axis_at - 1))

    factor_of = one(*split[0])
    for cut in split[1:]:
        factor_of = factor_of * one(*cut)
    return factor_of


def deal_out(stream_key, own, number, rows, count, top, reach, lean):
    sequence = jax.random.permutation(stream_key, count)
    heavy_load, ordinary = shares(count, rows * top, reach, lean, True), shares(count, rows * top, reach, lean, False)
    places = jnp.arange(count)

    def named(tallies, turn):
        used = int((tallies > 0).sum())
        fixed = max(1, used // 4)
        passed = fixed + (places - fixed + turn * (used - fixed)) % max(1, count - fixed)
        return jnp.zeros((count,), jnp.int32).at[sequence[jnp.where(places < fixed, places, passed)]].set(jnp.asarray(tallies, jnp.int32))

    tallies = jnp.where(number % 4 == 0, named(heavy_load, number // 4), named(ordinary, number - number // 4 - 1))
    mixed = jax.random.permutation(jax.random.fold_in(own, 3), count)
    giver, taker = mixed[0:count // 2 * 2:2], mixed[1:count // 2 * 2:2]
    margin = jnp.minimum(tallies[giver] - 1, reach - tallies[taker]) // 2
    margin = jnp.where((giver == sequence[0]) | (taker == sequence[0]) | (tallies[taker] == 0), 0, jnp.maximum(margin, 0))
    passed = jax.random.randint(jax.random.fold_in(own, 4), (count // 2,), 0, 1 << 20) % (margin + 1)
    tallies = tallies.at[giver].add(-passed).at[taker].add(passed)
    items = jnp.searchsorted(jnp.cumsum(tallies), jnp.arange(rows * top), side="right").astype(jnp.int32)
    grid = items.reshape(top, rows).T
    grid = grid[jax.random.permutation(jax.random.fold_in(own, 1), rows)]
    turn = jax.random.randint(jax.random.fold_in(own, 2), (rows, 1), 0, top)
    return jnp.take_along_axis(grid, (jnp.arange(top)[None, :] + turn) % top, axis=1)


def shares(number_of, total, bound, slope, full):
    loads = [(1 << 20) // math.isqrt(grade ** slope) + 1 for grade in range(1, number_of + 1)]
    largest = bound if full else min(bound, max(-(-total // number_of), total * loads[0] // sum(loads)))
    least = 1 if total - largest >= number_of - 1 else 0
    given, spare = [largest] + [least] * (number_of - 1), total - largest - least * (number_of - 1)
    while spare > 0:
        movable = [i for i in range(1, number_of) if given[i] < largest] or [i for i in range(1, number_of) if given[i] < bound]
        whole, budget = sum([loads[i] for i in movable]), spare
        for i in movable:
            extra = min(bound - given[i], max(1, budget * loads[i] // whole), spare)
            given[i] = given[i] + extra
            spare = spare - extra
    return np.array(given)


def bell_draw(key, extent, width, reach, split=(), held_as=jnp.bfloat16):
    values = width * jax.random.normal(key, extent, jnp.float32)
    if split:
        values = values * level_of(key, extent, split, -0.22, 0.18)
    return jnp.clip(values, -reach, reach).astype(held_as)


def setup_inputs(seed: int = 0) -> dict:
    key_of = jax.random.split(jax.random.key(seed), 16)
    filter_value = bell_draw(key_of[0], (MIX_TOKENS, CHANNELS), 1.0, 6.0, ((0, 32),))
    filter_gate = bell_draw(key_of[1], (MIX_TOKENS, CHANNELS), 1.5, 9.0, ((0, 32),))
    filter_taps = bell_draw(key_of[2], (TAPS, CHANNELS), TAPS ** -0.5, 1.0, (), jnp.float32)
    filter_bias = bell_draw(key_of[3], (CHANNELS,), 0.5, 3.0, (), jnp.float32)
    norm_gain = jnp.clip(1.0 + 0.18 * jax.random.normal(key_of[4], (CHANNELS,), jnp.float32), 0.1, 1.9)
    norm_shift = bell_draw(key_of[5], (CHANNELS,), 0.5, 3.0, (), jnp.float32)
    out_weight = bell_draw(key_of[6], (CHANNELS, D), CHANNELS ** -0.5, 0.1875)
    out_bias = bell_draw(key_of[7], (D,), 0.5, 3.0, (), jnp.float32)
    expert_input = bell_draw(key_of[8], (ROUTE_TOKENS, D), 1.0, 6.0, ((0, 8),))
    expert_gain = jnp.clip(1.0 + 0.18 * jax.random.normal(key_of[9], (D,), jnp.float32), 0.1, 1.9)
    route_experts_keys = jax.random.split(jax.random.fold_in(key_of[10], 1), ROUTE_TOKENS // ROUTE_DEV)
    route_experts_turns = jax.random.permutation(jax.random.fold_in(key_of[10], 3), ROUTE_TOKENS // ROUTE_DEV)
    route_experts = jax.vmap(lambda own, number: deal_out(jax.random.fold_in(key_of[10], 2), own, number, ROUTE_DEV, EXPERTS, TOPK, CAPACITY, 2))(route_experts_keys, route_experts_turns).reshape((ROUTE_TOKENS, TOPK))
    route_weights = jnp.clip(0.2 + 0.8 * jax.random.uniform(key_of[11], (ROUTE_TOKENS, TOPK), jnp.float32) ** level_of(key_of[11], (ROUTE_TOKENS, TOPK), ((0, 8),), -0.2, 0.2), 0.2, 1.0)
    gate_weights = bell_draw(key_of[12], (EXPERTS, D, HIDDEN_SIZE), (D // 8) ** -0.5, 0.375, ((0, 8), (2, 4)))
    up_weights = bell_draw(key_of[13], (EXPERTS, D, HIDDEN_SIZE), (D // 8) ** -0.5, 0.375, ((0, 8), (2, 4)))
    down_weights = bell_draw(key_of[14], (EXPERTS, HIDDEN_SIZE, D), (36 * HIDDEN_SIZE) ** -0.5, 0.0234375, ((0, 8), (1, 4)))
    return dict(filter_value=filter_value, filter_gate=filter_gate, filter_taps=filter_taps, filter_bias=filter_bias, norm_gain=norm_gain, norm_shift=norm_shift, out_weight=out_weight, out_bias=out_bias, expert_input=expert_input, expert_gain=expert_gain, route_experts=route_experts, route_weights=route_weights, gate_weights=gate_weights, up_weights=up_weights, down_weights=down_weights)


epsilon = 1e-06
clamp_limit = 7.0
swish_alpha = 1.702

def reference(filter_value, filter_gate, filter_taps, filter_bias, norm_gain, norm_shift, out_weight, out_bias, expert_input, expert_gain, route_experts, route_weights, gate_weights, up_weights, down_weights):
    gated = (filter_value.astype(jnp.float32) * jax.nn.sigmoid(filter_gate.astype(jnp.float32))).astype(jnp.bfloat16)
    length = gated.shape[0]
    padded = jnp.concatenate([jnp.zeros((TAPS - 1, CHANNELS), jnp.bfloat16), gated], 0)
    filtered = jnp.zeros((length, CHANNELS), jnp.float32)
    for offset in range(TAPS):
        filtered = filtered + filter_taps[offset] * padded[offset:offset + length].astype(jnp.float32)
    filtered = filtered + filter_bias
    average = lax.optimization_barrier(jnp.mean(filtered, 1, keepdims=True))
    centred = filtered - average
    variance = lax.optimization_barrier(jnp.mean(centred * centred, 1, keepdims=True))
    normed_filter = centred * lax.rsqrt(variance + epsilon) * norm_gain + norm_shift
    activated = jax.nn.silu(normed_filter).astype(jnp.bfloat16)
    mixer_out = (jnp.dot(activated, out_weight, preferred_element_type=jnp.float32) + out_bias).astype(jnp.bfloat16)
    token_values = expert_input.astype(jnp.float32)
    normed = (token_values * lax.rsqrt(lax.optimization_barrier(jnp.mean(token_values * token_values, 1, keepdims=True)) + epsilon) * expert_gain).astype(jnp.bfloat16)
    blocked = route_experts.reshape(N_EP, ROUTE_DEV * TOPK)
    onehot = (blocked[:, :, None] == jnp.arange(EXPERTS, dtype=jnp.int32)[None, None, :]).astype(jnp.int32)
    earlier = jnp.cumsum(onehot, 1) - onehot
    slot = lax.optimization_barrier(jnp.sum(earlier * onehot, 2)).astype(jnp.int32)
    row_slot = (jnp.arange(N_EP, dtype=jnp.int32)[:, None] * CAPACITY + slot).reshape(-1).astype(jnp.int32)
    flat_ids = route_experts.reshape(-1).astype(jnp.int32)
    copies = jnp.repeat(normed, TOPK, axis=0)
    buffer = jnp.zeros((EXPERTS, N_EP * CAPACITY, D), jnp.bfloat16).at[flat_ids, row_slot].set(copies)

    def expert_rows(operands):
        rows_in, gate_matrix, up_matrix, down_matrix = operands
        gate_pre = jnp.dot(rows_in, gate_matrix, preferred_element_type=jnp.float32)
        up_pre = jnp.dot(rows_in, up_matrix, preferred_element_type=jnp.float32)
        gate_held = jnp.minimum(gate_pre, clamp_limit)
        up_held = jnp.clip(up_pre, -clamp_limit, clamp_limit)
        hidden = (gate_held * jax.nn.sigmoid(swish_alpha * gate_held) * (up_held + 1.0)).astype(jnp.bfloat16)
        shards = hidden.reshape(-1, N_TP, HIDDEN_SIZE // N_TP).astype(jnp.float32)
        down_shards = down_matrix.reshape(N_TP, HIDDEN_SIZE // N_TP, D).astype(jnp.float32)
        partial_value = jnp.einsum('rpf,pfd->prd', shards, down_shards).astype(jnp.bfloat16)
        partial_value = lax.optimization_barrier(partial_value)
        return lax.optimization_barrier(jnp.sum(partial_value.astype(jnp.float32), 0)).astype(jnp.bfloat16)
    results = lax.map(expert_rows, (buffer, gate_weights, up_weights, down_weights))
    picked = results[flat_ids, row_slot].astype(jnp.float32).reshape(-1, TOPK, D)
    expert_out = lax.optimization_barrier(jnp.sum(picked * route_weights[:, :, None], 1)).astype(jnp.bfloat16)
    return (mixer_out, expert_out)
```

```python
import functools
import jax
import jax.numpy as jnp
from jax import lax
from jax.experimental import pallas as pl
from jax.experimental.pallas import tpu as pltpu
from jax.sharding import PartitionSpec as P

epsilon = 1e-06
clamp_limit = 7.0
swish_alpha = 1.702


def passed_along(array, axis, by):
    size = lax.axis_size(axis)
    pairs = [(i, i + by) for i in range(size) if 0 <= i + by < size]
    return lax.ppermute(array, axis, pairs)


def swapped(array, axis, mask):
    return lax.ppermute(array, axis, [(i, i ^ mask) for i in range(lax.axis_size(axis))])


def gated_filter(
    filter_value, filter_gate, filter_taps, filter_bias, norm_gain, norm_shift, out_weight, out_bias
):
    gated = (
        filter_value.astype(jnp.float32) * jax.nn.sigmoid(filter_gate.astype(jnp.float32))
    ).astype(jnp.bfloat16)
    length = gated.shape[0]
    reach_back = filter_taps.shape[0] - 1
    rim_rows = passed_along(gated[length - reach_back :], ("ep", "tp"), 1)
    padded = jnp.concatenate([rim_rows, gated], 0)
    filtered = jnp.zeros(gated.shape, jnp.float32)
    for offset in range(reach_back + 1):
        filtered = filtered + filter_taps[offset] * padded[offset : offset + length].astype(
            jnp.float32
        )
    filtered = filtered + filter_bias
    average = jnp.mean(filtered, 1, keepdims=True)
    centred = filtered - average
    variance = jnp.mean(centred * centred, 1, keepdims=True)
    normed_filter = centred * lax.rsqrt(variance + epsilon) * norm_gain + norm_shift
    activated = jax.nn.silu(normed_filter).astype(jnp.bfloat16)
    return (jnp.dot(activated, out_weight, preferred_element_type=jnp.float32) + out_bias).astype(
        jnp.bfloat16
    )


def expert_body(order, *refs, parts, blocks):
    xs, (gate_ref, up_ref, down_ref), rest = refs[:parts], refs[parts : parts + 3], refs[parts + 3 :]
    outs, acc = rest[:-1], rest[-1]
    width = xs[0].shape[1]
    step = pl.program_id(0)
    gate_pre = up_pre = 0.0
    for j in range(parts):
        rows = pl.ds(pl.multiple_of(order[j] * width, width), width)
        gate_pre += jnp.dot(xs[j][...], gate_ref[rows, :], preferred_element_type=jnp.float32)
        up_pre += jnp.dot(xs[j][...], up_ref[rows, :], preferred_element_type=jnp.float32)
    gate_held = jnp.minimum(gate_pre, clamp_limit)
    up_held = jnp.clip(up_pre, -clamp_limit, clamp_limit)
    hidden = (gate_held * jax.nn.sigmoid(swish_alpha * gate_held) * (up_held + 1.0)).astype(
        jnp.bfloat16
    )
    places = []
    for out in outs:
        places += [(out, k * width) for k in range(out.shape[1] // width)]
    for j, (out, at) in enumerate(places):
        cols = pl.ds(pl.multiple_of(order[j] * width, width), width)
        piece = jnp.dot(hidden, down_ref[:, cols], preferred_element_type=jnp.float32)
        mine = slice(j * width, (j + 1) * width)

        @pl.when(step == 0)
        def _():
            acc[:, mine] = piece

        @pl.when((step > 0) & (step < blocks - 1))
        def _():
            acc[:, mine] += piece

        @pl.when(step == blocks - 1)
        def _():
            out[:, at : at + width] = (acc[:, mine] + piece).astype(out.dtype)


def expert_products(order, pieces, gate, up, down, blocks=2):
    parts = len(pieces)
    rows, width = pieces[0].shape
    model, hid = gate.shape
    hb = hid // blocks
    widths = [width]
    while sum(widths) < model:
        widths.append(sum(widths))
    whole = lambda shape: pl.BlockSpec(shape, lambda i, order: (0, 0))
    return pl.pallas_call(
        functools.partial(expert_body, parts=parts, blocks=blocks),
        grid_spec=pltpu.PrefetchScalarGridSpec(
            num_scalar_prefetch=1,
            grid=(blocks,),
            in_specs=[whole((rows, width))] * parts
            + [pl.BlockSpec((model, hb), lambda i, order: (0, i))] * 2
            + [pl.BlockSpec((hb, model), lambda i, order: (i, 0))],
            out_specs=[whole((rows, w)) for w in widths],
            scratch_shapes=[pltpu.VMEM((rows, model), jnp.float32)],
        ),
        out_shape=[jax.ShapeDtypeStruct((rows, w), jnp.bfloat16) for w in widths],
        compiler_params=pltpu.CompilerParams(
            dimension_semantics=("arbitrary",), vmem_limit_bytes=40 * 1024 * 1024
        ),
        cost_estimate=pl.CostEstimate(
            flops=6 * rows * model * hid, bytes_accessed=6 * model * hid, transcendentals=rows * hid
        ),
        name="experts",
    )(order, *pieces, gate, up, down)


def routed_experts(
    expert_input, expert_gain, route_experts, route_weights, gate_weights, up_weights, down_weights
):
    row_count, per_token = route_experts.shape
    model_width = expert_input.shape[1]
    experts, shards = lax.axis_size("ep"), lax.axis_size("tp")
    me, part = lax.axis_index("ep"), lax.axis_index("tp")
    width = model_width // shards
    capacity = 2 * row_count * per_token // experts
    chunks = 2 if capacity % 32 == 0 else 1
    span = capacity // chunks

    token_values = expert_input.astype(jnp.float32)
    scale = lax.rsqrt(jnp.mean(token_values * token_values, 1, keepdims=True) + epsilon)
    own_values = lax.dynamic_slice_in_dim(expert_input, part * width, width, 1)
    own_gain = lax.dynamic_slice_in_dim(expert_gain, part * width, width, 0)
    normed = (own_values.astype(jnp.float32) * scale * own_gain).astype(jnp.bfloat16)

    relative = (route_experts ^ me).T
    named = relative[:, None, :] == jnp.arange(experts, dtype=jnp.int32)[None, :, None]
    member = jnp.any(named, 0)
    weight_of = jnp.sum(jnp.where(named, route_weights.T[:, None, :], 0.0), 0)
    places = jnp.arange(row_count, dtype=jnp.int32)
    before = (places[:, None] < places[None, :]).astype(jnp.bfloat16)
    earlier = jnp.dot(
        member.astype(jnp.bfloat16), before, preferred_element_type=jnp.float32
    ).astype(jnp.int32)
    slot = jnp.where(member, earlier, -1)

    def taken(chunk):
        seats = chunk * span + jnp.arange(span, dtype=jnp.int32)
        return slot[:, None, :] == seats[None, :, None]

    strides = [1 << b for b in reversed(range(shards.bit_length() - 1))]
    masks = [0]
    for stride in strides:
        masks = masks + [m ^ stride for m in masks]
    order = jnp.stack([part ^ m for m in masks]).astype(jnp.int32)

    arrivals = []
    for chunk in range(chunks):
        pick = taken(chunk).reshape(experts * span, row_count).astype(jnp.bfloat16)
        outgoing = jnp.dot(pick, normed, preferred_element_type=jnp.float32).astype(jnp.bfloat16)
        outgoing = outgoing.reshape(experts, span, width)
        arrivals.append(
            [outgoing[0]] + [swapped(outgoing[s], "ep", s) for s in range(1, experts)]
        )
    gathered = []
    for got in arrivals:
        pieces = [jnp.concatenate(got, 0)]
        for stride in strides:
            pieces = pieces + [swapped(p, "tp", stride) for p in pieces]
        gathered.append(pieces)
    returned = []
    for pieces in gathered:
        held = list(
            expert_products(order, pieces, gate_weights[0], up_weights[0], down_weights[0])
        )
        for stride in reversed(strides):
            received = swapped(held.pop(), "tp", stride)
            at = 0
            for k, mine in enumerate(held):
                w = mine.shape[1]
                held[k] = (
                    mine.astype(jnp.float32) + received[:, at : at + w].astype(jnp.float32)
                ).astype(jnp.bfloat16)
                at += w
        summed = held[0].reshape(experts, span, width)
        returned.append(
            [summed[0]] + [swapped(summed[s], "ep", s) for s in range(1, experts)]
        )
    total = 0.0
    for chunk, back in enumerate(returned):
        share = jnp.where(taken(chunk), weight_of[:, None, :], 0.0)
        share = share.reshape(experts * span, row_count)
        rounded = lax.reduce_precision(share, 8, 7)
        high, low = rounded.astype(jnp.bfloat16), (share - rounded).astype(jnp.bfloat16)
        values = jnp.concatenate(back, 0)
        for weights in (high, low):
            total = total + lax.dot_general(
                weights, values, (((0,), (0,)), ((), ())), preferred_element_type=jnp.float32
            )
    return total.astype(jnp.bfloat16)


def local(
    filter_value,
    filter_gate,
    filter_taps,
    filter_bias,
    norm_gain,
    norm_shift,
    out_weight,
    out_bias,
    expert_input,
    expert_gain,
    route_experts,
    route_weights,
    gate_weights,
    up_weights,
    down_weights,
):
    mixer_out = gated_filter(
        filter_value,
        filter_gate,
        filter_taps,
        filter_bias,
        norm_gain,
        norm_shift,
        out_weight,
        out_bias,
    )
    expert_out = routed_experts(
        expert_input,
        expert_gain,
        route_experts,
        route_weights,
        gate_weights,
        up_weights,
        down_weights,
    )
    return (mixer_out, expert_out)


def solution(mesh):
    in_specs = (
        P(("ep", "tp"), None),
        P(("ep", "tp"), None),
        P(),
        P(),
        P(),
        P(),
        P(),
        P(),
        P("ep", None),
        P(),
        P("ep", None),
        P("ep", None),
        P("ep", None, "tp"),
        P("ep", None, "tp"),
        P("ep", "tp", None),
    )
    out_specs = (P(("ep", "tp"), None), P("ep", "tp"))
    return jax.shard_map(local, mesh=mesh, in_specs=in_specs, out_specs=out_specs, check_vma=False)
```

```python
import functools
import jax
import jax.numpy as jnp
from jax import lax
from jax.experimental import pallas as pl
from jax.experimental.pallas import tpu as pltpu
from jax.sharding import PartitionSpec as P


epsilon = 1e-06
clamp_limit = 7.0
swish_alpha = 1.702


def passed_along(array, axis, by):
    size = lax.axis_size(axis)
    pairs = [(i, i + by) for i in range(size) if 0 <= i + by < size]
    return lax.ppermute(array, axis, pairs)


def swapped(array, axis, mask):
    pairs = [(i, i ^ mask) for i in range(lax.axis_size(axis))]
    return lax.ppermute(array, axis, pairs)


def gated_filter(
    filter_value, filter_gate, filter_taps, filter_bias, norm_gain, norm_shift, out_weight, out_bias
):
    gated = (
        filter_value.astype(jnp.float32) * jax.nn.sigmoid(filter_gate.astype(jnp.float32))
    ).astype(jnp.bfloat16)
    length = gated.shape[0]
    reach_back = filter_taps.shape[0] - 1
    rim_rows = passed_along(gated[length - reach_back :], ("ep", "tp"), 1)
    padded = jnp.concatenate([rim_rows, gated], 0)
    filtered = jnp.zeros(gated.shape, jnp.float32)
    for offset in range(reach_back + 1):
        filtered = filtered + filter_taps[offset] * padded[offset : offset + length].astype(
            jnp.float32
        )
    filtered = filtered + filter_bias
    average = jnp.mean(filtered, 1, keepdims=True)
    centred = filtered - average
    variance = jnp.mean(centred * centred, 1, keepdims=True)
    normed_filter = centred * lax.rsqrt(variance + epsilon) * norm_gain + norm_shift
    activated = jax.nn.silu(normed_filter).astype(jnp.bfloat16)
    return (jnp.dot(activated, out_weight, preferred_element_type=jnp.float32) + out_bias).astype(
        jnp.bfloat16
    )


def expert_body(order, *refs, parts, outs_n):
    xs, (gate_ref, up_ref, down_ref) = refs[:parts], refs[parts : parts + 3]
    outs = refs[parts + 3 : parts + 3 + outs_n]
    gate_buf, up_buf, down_buf, sems = refs[parts + 3 + outs_n :]
    width = xs[0].shape[1]
    blocks, _, hb = gate_buf.shape
    loads = []
    for i in range(blocks):
        mine = pl.ds(i * hb, hb)
        loads.append(pltpu.make_async_copy(gate_ref.at[:, mine], gate_buf.at[i], sems.at[2 * i]))
        loads.append(pltpu.make_async_copy(up_ref.at[:, mine], up_buf.at[i], sems.at[2 * i + 1]))
    loads.append(pltpu.make_async_copy(down_ref, down_buf, sems.at[2 * blocks]))
    for load in loads:
        load.start()
    hidden = []
    for i in range(blocks):
        sides = []
        for buf, load in ((gate_buf, loads[2 * i]), (up_buf, loads[2 * i + 1])):
            load.wait()
            total = 0.0
            for j in range(parts):
                rows = pl.ds(pl.multiple_of(order[j] * width, width), width)
                total += jnp.dot(xs[j][...], buf[i, rows, :], preferred_element_type=jnp.float32)
            sides.append(total)
        gate_held = jnp.minimum(sides[0], clamp_limit)
        up_held = jnp.clip(sides[1], -clamp_limit, clamp_limit)
        hidden.append(
            (gate_held * jax.nn.sigmoid(swish_alpha * gate_held) * (up_held + 1.0)).astype(
                jnp.bfloat16
            )
        )
    hidden = jnp.concatenate(hidden, 1)
    loads[-1].wait()
    places = []
    for out in outs:
        places += [(out, k * width) for k in range(out.shape[1] // width)]
    for j, (out, at) in enumerate(places):
        cols = pl.ds(pl.multiple_of(order[j] * width, width), width)
        out[:, at : at + width] = jnp.dot(
            hidden, down_buf[:, cols], preferred_element_type=jnp.float32
        ).astype(out.dtype)


def expert_products(order, pieces, gate, up, down, blocks=2):
    parts = len(pieces)
    rows, width = pieces[0].shape
    model, hid = gate.shape
    widths = [width]
    while sum(widths) < model:
        widths.append(sum(widths))
    return pl.pallas_call(
        functools.partial(expert_body, parts=parts, outs_n=len(widths)),
        in_specs=[pl.BlockSpec(memory_space=pltpu.SMEM)]
        + [pl.BlockSpec(memory_space=pltpu.VMEM)] * parts
        + [pl.BlockSpec(memory_space=pl.ANY)] * 3,
        out_shape=[jax.ShapeDtypeStruct((rows, w), jnp.bfloat16) for w in widths],
        scratch_shapes=[pltpu.VMEM((blocks, model, hid // blocks), jnp.bfloat16)] * 2
        + [pltpu.VMEM((hid, model), jnp.bfloat16), pltpu.SemaphoreType.DMA((2 * blocks + 1,))],
        compiler_params=pltpu.CompilerParams(vmem_limit_bytes=32 * 1024 * 1024),
        cost_estimate=pl.CostEstimate(
            flops=6 * rows * model * hid, bytes_accessed=6 * model * hid, transcendentals=rows * hid
        ),
        name="experts",
    )(order, *pieces, gate, up, down)


def dispatch_body(
    at_ref, values_ref, gain_ref, route_ref, pos_ref, *outs, experts, capacity, span, width
):
    values = values_ref[...].astype(jnp.float32)
    scale = lax.rsqrt(jnp.mean(values * values, 1, keepdims=True) + epsilon)
    cols = pl.ds(pl.multiple_of(at_ref[1] * width, width), width)
    normed = (values_ref[:, cols].astype(jnp.float32) * scale * gain_ref[:, cols]).astype(
        jnp.bfloat16
    )
    count, per_token = route_ref.shape
    relative = route_ref[...] ^ at_ref[0]
    lane = lax.broadcasted_iota(jnp.int32, (count, experts), 1)
    hits = [relative[:, k : k + 1] == lane for k in range(per_token)]
    member = functools.reduce(jnp.logical_or, hits)
    here = lax.broadcasted_iota(jnp.int32, (count, count), 0)
    there = lax.broadcasted_iota(jnp.int32, (count, count), 1)
    before = jnp.where(there < here, 1.0, 0.0).astype(jnp.bfloat16)
    earlier = jnp.dot(
        before,
        jnp.where(member, 1.0, 0.0).astype(jnp.bfloat16),
        preferred_element_type=jnp.float32,
    )
    seat = lax.broadcasted_iota(jnp.int32, (count, experts * capacity), 1)
    pick = None
    for k in range(per_token):
        slot = jnp.sum(jnp.where(hits[k], earlier, 0.0), 1, keepdims=True).astype(jnp.int32)
        pos = relative[:, k : k + 1] * capacity + slot
        pos_ref[:, k : k + 1] = pos
        pick = seat == pos if pick is None else pick | (seat == pos)
    outgoing = lax.dot_general(
        jnp.where(pick, 1.0, 0.0).astype(jnp.bfloat16),
        normed,
        (((0,), (0,)), ((), ())),
        preferred_element_type=jnp.float32,
    ).astype(jnp.bfloat16)
    for n, out in enumerate(outs):
        start = (n % experts) * capacity + (n // experts) * span
        out[...] = outgoing[start : start + span]


def join_body(*refs):
    out = refs[-1]
    span = refs[0].shape[0]
    for n, ref in enumerate(refs[:-1]):
        out[n * span : (n + 1) * span, :] = ref[...]


def joined(pieces):
    span, width = pieces[0].shape
    return pl.pallas_call(
        join_body, out_shape=jax.ShapeDtypeStruct((span * len(pieces), width), jnp.bfloat16)
    )(*pieces)


def combine_body(pos_ref, weights_ref, *refs, experts, capacity, span):
    pieces, out, scratch = refs[:-2], refs[-2], refs[-1]
    count, per_token = pos_ref.shape
    total = 0.0
    for chunk in range(capacity // span):
        for s in range(experts):
            scratch[s * span : (s + 1) * span, :] = pieces[chunk * experts + s][...]
        lane = lax.broadcasted_iota(jnp.int32, (count, experts * span), 1)
        seat = lane // span * capacity + chunk * span + lane % span
        share = 0.0
        for k in range(per_token):
            share += jnp.where(seat == pos_ref[:, k : k + 1], weights_ref[:, k : k + 1], 0.0)
        high = share.astype(jnp.bfloat16)
        low = (share - high.astype(jnp.float32)).astype(jnp.bfloat16)
        for part in (high, low):
            total += jnp.dot(part, scratch[...], preferred_element_type=jnp.float32)
    out[...] = total.astype(jnp.bfloat16)


def routed_experts(
    expert_input, expert_gain, route_experts, route_weights, gate_weights, up_weights, down_weights
):
    row_count, per_token = route_experts.shape
    model_width = expert_input.shape[1]
    experts, shards = lax.axis_size("ep"), lax.axis_size("tp")
    me, part = lax.axis_index("ep"), lax.axis_index("tp")
    width = model_width // shards
    capacity = 2 * row_count * per_token // experts
    chunks = 2 if capacity % 32 == 0 else 1
    span = capacity // chunks

    sends = pl.pallas_call(
        functools.partial(
            dispatch_body, experts=experts, capacity=capacity, span=span, width=width
        ),
        in_specs=[pl.BlockSpec(memory_space=pltpu.SMEM)]
        + [pl.BlockSpec(memory_space=pltpu.VMEM)] * 3,
        out_shape=[jax.ShapeDtypeStruct((row_count, per_token), jnp.int32)]
        + [jax.ShapeDtypeStruct((span, width), jnp.bfloat16)] * (experts * chunks),
        name="dispatch",
    )(
        jnp.stack([me, part]).astype(jnp.int32),
        expert_input,
        expert_gain.reshape(1, -1),
        route_experts,
    )
    pos, sends = sends[0], sends[1:]

    strides = [1 << b for b in reversed(range(shards.bit_length() - 1))]
    masks = [0]
    for stride in strides:
        masks = masks + [m ^ stride for m in masks]
    order = jnp.stack([part ^ m for m in masks]).astype(jnp.int32)

    arrivals = []
    for chunk in range(chunks):
        outgoing = sends[chunk * experts : (chunk + 1) * experts]
        far_first = [swapped(outgoing[s], "ep", s) for s in range(experts - 1, 0, -1)]
        arrivals.append([outgoing[0]] + far_first[::-1])
    gathered = []
    for got in arrivals:
        pieces = [joined(got)]
        for stride in strides:
            pieces = pieces + [swapped(p, "tp", stride) for p in pieces]
        gathered.append(pieces)
    returned = []
    for pieces in gathered:
        held = list(expert_products(order, pieces, gate_weights[0], up_weights[0], down_weights[0]))
        for stride in reversed(strides):
            received = swapped(held.pop(), "tp", stride)
            at = 0
            for k, mine in enumerate(held):
                w = mine.shape[1]
                held[k] = (
                    mine.astype(jnp.float32) + received[:, at : at + w].astype(jnp.float32)
                ).astype(jnp.bfloat16)
                at += w
        summed = held[0].reshape(experts, span, width)
        far_first = [swapped(summed[s], "ep", s) for s in range(experts - 1, 0, -1)]
        returned += [summed[0]] + far_first[::-1]
    return pl.pallas_call(
        functools.partial(combine_body, experts=experts, capacity=capacity, span=span),
        out_shape=jax.ShapeDtypeStruct((row_count, width), jnp.bfloat16),
        scratch_shapes=[pltpu.VMEM((experts * span, width), jnp.bfloat16)],
        name="combine",
    )(pos, route_weights, *returned)


def local(
    filter_value,
    filter_gate,
    filter_taps,
    filter_bias,
    norm_gain,
    norm_shift,
    out_weight,
    out_bias,
    expert_input,
    expert_gain,
    route_experts,
    route_weights,
    gate_weights,
    up_weights,
    down_weights,
):
    mixer_out = gated_filter(
        filter_value,
        filter_gate,
        filter_taps,
        filter_bias,
        norm_gain,
        norm_shift,
        out_weight,
        out_bias,
    )
    expert_out = routed_experts(
        expert_input,
        expert_gain,
        route_experts,
        route_weights,
        gate_weights,
        up_weights,
        down_weights,
    )
    return (mixer_out, expert_out)


def solution(mesh):
    in_specs = (
        P(("ep", "tp"), None),
        P(("ep", "tp"), None),
        P(),
        P(),
        P(),
        P(),
        P(),
        P(),
        P("ep", None),
        P(),
        P("ep", None),
        P("ep", None),
        P("ep", None, "tp"),
        P("ep", None, "tp"),
        P("ep", "tp", None),
    )
    out_specs = (P(("ep", "tp"), None), P("ep", "tp"))
    return jax.shard_map(
        local, mesh=mesh, in_specs=in_specs, out_specs=out_specs, check_vma=False
    )
```
